32 devices in a mesh: rep: 2 (over y), fs: 4 (over z), tp: 4 (over x, core).
Axes of the slice: x: 2, y: 2, z: 4, core: 2. Of those that a mesh axis runs over, the one named last changes fastest.
Arguments:
- tokens: bfloat16 [4096, 2048], P(('rep', 'fs'), 'tp'), may hold values from -6 to 6
- pre_gain: float32 [2048], replicated, may hold values from 0.1 to 1.9
- u_weight: float32 [2048, 512], P('fs', 'tp'), may hold values from -0.125 to 0.125
- u_scale: float32 [512], P('tp'), may hold values from 0.5 to 2
- v_weight: float32 [2048, 512], P('fs', 'tp'), may hold values from -0.125 to 0.125
- v_scale: float32 [512], P('tp'), may hold values from 0.5 to 2
- group_gain: float32 [512], P('tp'), may hold values from 0.1 to 1.9
- span_weight: bfloat16 [8, 128, 128], P('tp'), may hold values from -0.5 to 0.5
- span_bias: float32 [8, 128], P('tp'), may hold values from 0.5 to 1.5
- out_weight: float32 [512, 2048], P('tp', 'fs'), may hold values from -0.25 to 0.25
- out_scale: float32 [2048], P('fs'), may hold values from 0.5 to 2
- ffn_gain: float32 [2048], replicated, may hold values from 0.1 to 1.9
- gate_weight: float32 [2048, 5632], P('fs', 'tp'), may hold values from -0.125 to 0.125
- gate_scale: float32 [5632], P('tp'), may hold values from 0.5 to 2
- up_weight: float32 [2048, 5632], P('fs', 'tp'), may hold values from -0.125 to 0.125
- up_scale: float32 [5632], P('tp'), may hold values from 0.5 to 2
- down_weight: float32 [5632, 2048], P('tp', 'fs'), may hold values from -0.078125 to 0.078125
- down_scale: float32 [2048], P('fs'), may hold values from 0.5 to 2
Outputs:
- layer_out: bfloat16 [4096, 2048], P(('rep', 'fs'), 'tp')
The draws below stay inside these ranges and needn't reach their ends.
All inputs are finite; a program needn't handle non-finite values.
Results may differ from the reference program's by a relative error of at most 0.02.
Values may be sent and summed in bfloat16 or wider, within the bound.
A program may use at most 64 MiB of HBM per device.

```python
import math
import jax
import jax.numpy as jnp
from jax import lax

D = 2048
GROUPS = 8
GROUP_DIM = 64
MIX_WIDTH = 512
HIDDEN_SIZE = 5632
SPAN = 128
TOKENS = 4096
N_TP = 4


def levels(rng, shape, shards, smallest, largest):
    def one(dim, shards_of):
        steps = jax.random.uniform(jax.random.fold_in(jax.random.fold_in(rng, 6), dim), (shards_of,), jnp.float32, smallest / len(shards), largest / len(shards))
        return jnp.repeat(jnp.exp(steps), shape[dim] // shards_of).reshape((-1,) + (1,) * (len(shape) - dim - 1))

    level = one(*shards[0])
    for cut in shards[1:]:
        level = level * one(*cut)
    return level


def normal_values(key, extent, scale, reach, shards=(), held_as=jnp.bfloat16):
    entries = jax.random.normal(key, extent, jnp.float32) * scale
    if len(shards) > 0:
        entries = levels(key, extent, shards, -0.22, 0.18) * entries
    return jnp.clip(entries, min=-reach, max=reach).astype(held_as)


def setup_inputs(seed: int = 0) -> dict:
    arg_keys = jax.random.split(jax.random.key(seed), 19)
    tokens = normal_values(arg_keys[0], (TOKENS, D), 1.0, 6.0, ((0, 8), (1, 4)))
    pre_gain = jnp.clip(1.0 + 0.18 * jax.random.normal(arg_keys[1], (D,), jnp.float32), 0.1, 1.9)
    u_weight = normal_values(arg_keys[2], (D, MIX_WIDTH), D ** -0.5, 0.125, ((0, 4), (1, 4)), jnp.float32)
    u_scale = jnp.clip(jnp.exp(math.log(2.0) - 1.3862944 * jax.random.uniform(arg_keys[3], (MIX_WIDTH,), jnp.float32) ** levels(arg_keys[3], (MIX_WIDTH,), ((0, 4),), -0.2, 0.2)), 0.5, 2.0)
    v_weight = normal_values(arg_keys[4], (D, MIX_WIDTH), D ** -0.5, 0.125, ((0, 4), (1, 4)), jnp.float32)
    v_scale = jnp.clip(jnp.exp(math.log(2.0) - 1.3862944 * jax.random.uniform(arg_keys[5], (MIX_WIDTH,), jnp.float32) ** levels(arg_keys[5], (MIX_WIDTH,), ((0, 4),), -0.2, 0.2)), 0.5, 2.0)
    group_gain = jnp.clip(1.0 + 0.18 * jax.random.normal(arg_keys[6], (MIX_WIDTH,), jnp.float32), 0.1, 1.9)
    span_weight = normal_values(arg_keys[7], (GROUPS, SPAN, SPAN), SPAN ** -0.5, 0.5, ((0, 4),))
    span_bias = jnp.clip(0.5 + 1.0 * jax.random.uniform(arg_keys[8], (GROUPS, SPAN), jnp.float32) ** levels(arg_keys[8], (GROUPS, SPAN), ((0, 4),), -0.2, 0.2), 0.5, 1.5)
    out_weight = normal_values(arg_keys[9], (MIX_WIDTH, D), MIX_WIDTH ** -0.5, 0.25, ((0, 4), (1, 4)), jnp.float32)
    out_scale = jnp.clip(jnp.exp(math.log(2.0) - 1.3862944 * jax.random.uniform(arg_keys[10], (D,), jnp.float32) ** levels(arg_keys[10], (D,), ((0, 4),), -0.2, 0.2)), 0.5, 2.0)
    ffn_gain = jnp.clip(1.0 + 0.18 * jax.random.normal(arg_keys[11], (D,), jnp.float32), 0.1, 1.9)
    gate_weight = normal_values(arg_keys[12], (D, HIDDEN_SIZE), D ** -0.5, 0.125, ((0, 4), (1, 4)), jnp.float32)
    gate_scale = jnp.clip(jnp.exp(math.log(2.0) - 1.3862944 * jax.random.uniform(arg_keys[13], (HIDDEN_SIZE,), jnp.float32) ** levels(arg_keys[13], (HIDDEN_SIZE,), ((0, 4),), -0.2, 0.2)), 0.5, 2.0)
    up_weight = normal_values(arg_keys[14], (D, HIDDEN_SIZE), D ** -0.5, 0.125, ((0, 4), (1, 4)), jnp.float32)
    up_scale = jnp.clip(jnp.exp(math.log(2.0) - 1.3862944 * jax.random.uniform(arg_keys[15], (HIDDEN_SIZE,), jnp.float32) ** levels(arg_keys[15], (HIDDEN_SIZE,), ((0, 4),), -0.2, 0.2)), 0.5, 2.0)
    down_weight = normal_values(arg_keys[16], (HIDDEN_SIZE, D), HIDDEN_SIZE ** -0.5, 0.078125, ((0, 4), (1, 4)), jnp.float32)
    down_scale = jnp.clip(jnp.exp(math.log(2.0) - 1.3862944 * jax.random.uniform(arg_keys[17], (D,), jnp.float32) ** levels(arg_keys[17], (D,), ((0, 4),), -0.2, 0.2)), 0.5, 2.0)
    return {"tokens": tokens, "pre_gain": pre_gain, "u_weight": u_weight, "u_scale": u_scale, "v_weight": v_weight, "v_scale": v_scale, "group_gain": group_gain, "span_weight": span_weight, "span_bias": span_bias, "out_weight": out_weight, "out_scale": out_scale, "ffn_gain": ffn_gain, "gate_weight": gate_weight, "gate_scale": gate_scale, "up_weight": up_weight, "up_scale": up_scale, "down_weight": down_weight, "down_scale": down_scale}


EPS = 0.02

def rms_rows(values, gain):
    wide = values.astype(jnp.float32)
    scaled = wide * lax.rsqrt(lax.optimization_barrier(jnp.mean(wide * wide, axis=-1, keepdims=True)) + EPS)
    return (scaled * gain).astype(jnp.bfloat16)

def block_sum(acts, weight, scale):
    width = acts.shape[1] // N_TP
    acts_blocks = jnp.moveaxis(acts.reshape(acts.shape[0], N_TP, width), 1, 0)
    weight_blocks = weight.astype(jnp.bfloat16).reshape(N_TP, width, weight.shape[1])

    def add_block(total, pair):
        term = (jnp.dot(pair[0], pair[1], preferred_element_type=jnp.float32) * scale).astype(jnp.bfloat16)
        return (total + term.astype(jnp.float32), None)
    start = jnp.zeros((acts.shape[0], weight.shape[1]), jnp.float32)
    total, unused = lax.scan(add_block, start, (acts_blocks, weight_blocks))
    return total.astype(jnp.bfloat16)

def reference(tokens, pre_gain, u_weight, u_scale, v_weight, v_scale, group_gain, span_weight, span_bias, out_weight, out_scale, ffn_gain, gate_weight, gate_scale, up_weight, up_scale, down_weight, down_scale):
    row_count = tokens.shape[0]
    normed = rms_rows(tokens, pre_gain)
    u_act = jax.nn.gelu(jnp.dot(normed, u_weight.astype(jnp.bfloat16), preferred_element_type=jnp.float32) * u_scale)
    v_act = jax.nn.gelu(jnp.dot(normed, v_weight.astype(jnp.bfloat16), preferred_element_type=jnp.float32) * v_scale)
    grouped = v_act.reshape(row_count, GROUPS, GROUP_DIM)
    centre = lax.optimization_barrier(jnp.mean(grouped, axis=-1, keepdims=True))
    spread = lax.optimization_barrier(jnp.mean(jnp.square(grouped - centre), axis=-1, keepdims=True))
    v_norm = (((grouped - centre) * lax.rsqrt(spread + EPS)).reshape(row_count, MIX_WIDTH) * group_gain).astype(jnp.bfloat16)
    spans = v_norm.reshape(row_count // SPAN, SPAN, GROUPS, GROUP_DIM).astype(jnp.float32)
    lower = jnp.tril(span_weight).astype(jnp.float32)
    mixed = jnp.einsum('gts,nsgc->ntgc', lower, spans) + jnp.transpose(span_bias)[None, :, :, None]
    gated = (u_act * mixed.reshape(row_count, MIX_WIDTH)).astype(jnp.bfloat16)
    mix = (jnp.dot(gated, out_weight.astype(jnp.bfloat16), preferred_element_type=jnp.float32) * out_scale).astype(jnp.bfloat16)
    resid = (tokens.astype(jnp.float32) + mix.astype(jnp.float32)).astype(jnp.bfloat16)
    normed_ffn = rms_rows(resid, ffn_gain)
    gate_pre = jnp.dot(normed_ffn, gate_weight.astype(jnp.bfloat16), preferred_element_type=jnp.float32) * gate_scale
    up_pre = jnp.dot(normed_ffn, up_weight.astype(jnp.bfloat16), preferred_element_type=jnp.float32) * up_scale
    hidden = (jax.nn.silu(gate_pre) * up_pre).astype(jnp.bfloat16)
    ffn = block_sum(hidden, down_weight, down_scale)
    return (resid.astype(jnp.float32) + ffn.astype(jnp.float32)).astype(jnp.bfloat16)
```

```python
import jax
import jax.numpy as jnp
from jax import lax
from jax.sharding import PartitionSpec as P

EPS = 0.02


def rms_rows(values, gain):
    wide = values.astype(jnp.float32)
    scaled = wide * lax.rsqrt(jnp.mean(wide * wide, axis=-1, keepdims=True) + EPS)
    return (scaled * gain).astype(jnp.bfloat16)


def fold_pair(source, pieces):
    first = jnp.dot(source, pieces[0], preferred_element_type=jnp.float32)
    second = jnp.dot(source, pieces[1], preferred_element_type=jnp.float32)
    return (first, second)


def project_cols(source, scale_whole, piece):
    return jnp.dot(source, piece, preferred_element_type=jnp.float32) * scale_whole


def gather_shared(piece, axis):
    width = piece.shape[axis] // lax.axis_size("rep")
    part = lax.dynamic_slice_in_dim(piece, lax.axis_index("rep") * width, width, axis)
    return lax.all_gather(part, ("fs", "rep"), axis=axis, tiled=True)


def shards(
    tokens,
    pre_gain,
    u_weight,
    u_scale,
    v_weight,
    v_scale,
    group_gain,
    span_weight,
    span_bias,
    out_weight,
    out_scale,
    ffn_gain,
    gate_weight,
    gate_scale,
    up_weight,
    up_scale,
    down_weight,
    down_scale,
):
    gate_cast = gate_weight.astype(jnp.bfloat16)
    up_cast = up_weight.astype(jnp.bfloat16)
    full_rows = lax.all_gather(tokens, "tp", axis=1, tiled=True)
    row_count = full_rows.shape[0]
    normed = rms_rows(full_rows, pre_gain)
    u_pre, v_pre = fold_pair(
        normed,
        (
            lax.all_gather(u_weight.astype(jnp.bfloat16), "fs", axis=0, tiled=True),
            lax.all_gather(v_weight.astype(jnp.bfloat16), "fs", axis=0, tiled=True),
        ),
    )
    out_whole, down_whole = (
        lax.all_gather(out_scale, "fs", axis=0, tiled=True),
        lax.all_gather(down_scale, "fs", axis=0, tiled=True),
    )
    u_act = jax.nn.gelu(u_pre * u_scale)
    v_act = jax.nn.gelu(v_pre * v_scale)
    local_groups = span_weight.shape[0]
    span_len = span_weight.shape[1]
    group_width = v_act.shape[1] // local_groups
    grouped = v_act.reshape(row_count, local_groups, group_width)
    centre = jnp.mean(grouped, axis=-1, keepdims=True)
    spread = jnp.mean(jnp.square(grouped - centre), axis=-1, keepdims=True)
    v_norm = (
        ((grouped - centre) * lax.rsqrt(spread + EPS)).reshape(row_count, -1) * group_gain
    ).astype(jnp.bfloat16)
    spans = v_norm.reshape(row_count // span_len, span_len, local_groups, group_width)
    mixed = jnp.einsum(
        "gts,nsgc->ntgc", jnp.tril(span_weight), spans, preferred_element_type=jnp.float32
    )
    mixed = mixed + jnp.transpose(span_bias)[None, :, :, None]
    gated = (u_act * mixed.reshape(row_count, -1)).astype(jnp.bfloat16)
    out_cast = out_weight.astype(jnp.bfloat16)
    own_width = tokens.shape[1]
    gated_full = lax.all_gather(gated, "tp", axis=1, tiled=True)
    out_rows = lax.all_gather(out_cast, "fs", axis=1, tiled=True)
    out_own = lax.all_to_all(out_rows, "tp", split_axis=1, concat_axis=0, tiled=True)
    scale_own = lax.dynamic_slice_in_dim(out_whole, lax.axis_index("tp") * own_width, own_width, 0)
    mix_own = (jnp.dot(gated_full, out_own, preferred_element_type=jnp.float32) * scale_own).astype(
        jnp.bfloat16
    )
    resid_own = (tokens.astype(jnp.float32) + mix_own.astype(jnp.float32)).astype(jnp.bfloat16)
    resid_full = lax.all_gather(resid_own, "tp", axis=1, tiled=True)
    normed_ffn = rms_rows(resid_full, ffn_gain)
    gate_acc, up_acc = fold_pair(
        normed_ffn,
        (
            gather_shared(gate_cast, 0),
            gather_shared(up_cast, 0),
        ),
    )
    hidden = (jax.nn.silu(gate_acc * gate_scale) * (up_acc * up_scale)).astype(jnp.bfloat16)
    ffn_terms = project_cols(
        hidden,
        down_whole,
        gather_shared(down_weight.astype(jnp.bfloat16), 1),
    )
    ffn_own = lax.psum_scatter(
        ffn_terms.astype(jnp.bfloat16), "tp", scatter_dimension=1, tiled=True
    )
    return (resid_own.astype(jnp.float32) + ffn_own.astype(jnp.float32)).astype(jnp.bfloat16)


def solution(mesh):
    placed = (
        P(("rep", "fs"), "tp"),
        P(),
        P("fs", "tp"),
        P("tp"),
        P("fs", "tp"),
        P("tp"),
        P("tp"),
        P("tp", None, None),
        P("tp", None),
        P("tp", "fs"),
        P("fs"),
        P(),
        P("fs", "tp"),
        P("tp"),
        P("fs", "tp"),
        P("tp"),
        P("tp", "fs"),
        P("fs"),
    )
    return jax.shard_map(
        shards, mesh=mesh, in_specs=placed, out_specs=P(("rep", "fs"), "tp"), check_vma=False
    )
```

```python
import functools

import jax
import jax.numpy as jnp
from jax import lax
from jax.experimental import pallas as pl
from jax.experimental.pallas import tpu as pltpu
from jax.sharding import PartitionSpec as P

EPS = 0.02
MESH = pl.DeviceIdType.MESH
SCALES, MIXER_IN, MIXER_OUT, GATE, UP, DOWN_A, DOWN_B = range(7)
KINDS = 7
TOKENS, OUT_ROWS, GATED = range(3)


def layer_kernel(
    sizes,
    tokens_ref,
    scales_ref,
    uv_ref,
    out_ref,
    gate_ref,
    up_ref,
    down_ref,
    pre_gain_ref,
    ffn_gain_ref,
    u_scale_ref,
    v_scale_ref,
    group_gain_ref,
    lower_ref,
    bias_ref,
    gate_scale_ref,
    up_scale_ref,
    result_ref,
    tok_all,
    scale_all,
    uv_all,
    out_all,
    gate_all,
    up_all,
    down_all,
    normed,
    gated_all,
    gate_acc,
    up_acc,
    hidden,
    ffn_acc,
    part,
    parts_in,
    local_sem,
    ring_send,
    ring_recv,
    tp_send,
    tp_recv,
    part_send,
    part_recv,
):
    n_rep, n_fs, n_tp = sizes
    n_ring = n_rep * n_fs
    far, near = n_ring // 2, n_ring - 1 - n_ring // 2
    hops = {SCALES: (far, near), MIXER_IN: (far, near), MIXER_OUT: (near, far), GATE: (far, near),
            UP: (near, far), DOWN_A: (far, near), DOWN_B: (near, far)}
    rows, own_width = tokens_ref.shape
    block = normed.shape[2]
    per_own = own_width // block
    rep, fs, tp = lax.axis_index("rep"), lax.axis_index("fs"), lax.axis_index("tp")

    def place(r, f):
        return r * n_fs + jnp.where(lax.rem(r, 2) == 0, f, n_fs - 1 - f)

    def coords(q):
        r, f = q // n_fs, lax.rem(q, n_fs)
        return r, jnp.where(lax.rem(r, 2) == 0, f, n_fs - 1 - f)

    me = place(rep, fs)

    def at_hop(way, hop):
        return lax.rem(me - hop + n_ring, n_ring) if way == 0 else lax.rem(me + hop, n_ring)

    def ring_id(way):
        r, f = coords(at_hop(1 - way, 1))
        return {"rep": r, "fs": f}

    uv_rows, out_rows, down_rows = uv_ref.shape[1], out_ref.shape[0], down_ref.shape[0]
    half = down_rows // 2

    def slot(kind, q):
        r, f = coords(q)
        if kind == SCALES:
            return scale_all.at[q]
        if kind == MIXER_IN:
            return uv_all.at[f, :, pl.ds(pl.multiple_of(r * uv_rows, uv_rows), uv_rows)]
        if kind == MIXER_OUT:
            return out_all.at[f, tp, pl.ds(pl.multiple_of(r * out_rows, out_rows), out_rows)]
        if kind == GATE:
            return gate_all.at[q]
        if kind == UP:
            return up_all.at[q]
        return down_all.at[q, pl.ds(0 if kind == DOWN_A else half, half)]

    def send(kind, way, hop):
        ref = slot(kind, at_hop(way, hop - 1))
        return pltpu.make_async_remote_copy(
            src_ref=ref, dst_ref=ref, send_sem=ring_send.at[kind, way, hop - 1],
            recv_sem=ring_recv.at[kind, way, hop - 1], device_id=ring_id(way), device_id_type=MESH)

    def wait_hop(kind, way, hop):
        ref = slot(kind, at_hop(way, hop))
        pltpu.make_async_remote_copy(
            src_ref=ref, dst_ref=ref, send_sem=ring_send.at[kind, way, hop - 1],
            recv_sem=ring_recv.at[kind, way, hop - 1], device_id=ring_id(way),
            device_id_type=MESH).wait_recv()

    def on(condition, action):
        if isinstance(condition, bool):
            if condition:
                action()
        else:
            pl.when(condition)(action)

    def begin(kind):
        for way in range(2):
            send(kind, way, 1).start()

    def pump(kind, hop):
        for way in range(2):
            def take(way=way):
                wait_hop(kind, way, hop)
                on(hop < hops[kind][way], lambda: send(kind, way, hop + 1).start())
            on(hop <= hops[kind][way], take)

    def tp_ref(kind, t):
        if kind == TOKENS:
            return tok_all.at[t]
        if kind == OUT_ROWS:
            return out_all.at[:, t]
        return gated_all.at[t]

    def tp_copy(kind, k, t):
        ref = tp_ref(kind, t)
        return pltpu.make_async_remote_copy(
            src_ref=ref, dst_ref=ref, send_sem=tp_send.at[kind, k - 1],
            recv_sem=tp_recv.at[kind, k - 1], device_id={"tp": lax.rem(tp + k, n_tp)},
            device_id_type=MESH)

    def tp_start(kind):
        for k in range(1, n_tp):
            tp_copy(kind, k, tp).start()

    def tp_wait(kind):
        for k in range(1, n_tp):
            tp_copy(kind, k, lax.rem(tp - k + n_tp, n_tp)).wait_recv()

    own = [
        pltpu.make_async_copy(tokens_ref, tok_all.at[tp], local_sem.at[0]),
        pltpu.make_async_copy(scales_ref, slot(SCALES, me), local_sem.at[1]),
        pltpu.make_async_copy(uv_ref, slot(MIXER_IN, me), local_sem.at[2]),
        pltpu.make_async_copy(out_ref, slot(MIXER_OUT, me), local_sem.at[3]),
        pltpu.make_async_copy(gate_ref, gate_all.at[me], local_sem.at[4]),
        pltpu.make_async_copy(up_ref, up_all.at[me], local_sem.at[5]),
        pltpu.make_async_copy(down_ref, down_all.at[me], local_sem.at[6]),
    ]
    for copy in own:
        copy.start()
    barrier = pltpu.get_barrier_semaphore()
    for way in range(2):
        pl.semaphore_signal(barrier, inc=1, device_id=ring_id(way), device_id_type=MESH)
    for k in range(1, n_tp):
        pl.semaphore_signal(barrier, inc=1, device_id={"tp": lax.rem(tp + k, n_tp)},
                            device_id_type=MESH)
    pl.semaphore_wait(barrier, 2 + n_tp - 1)
    for copy in own:
        copy.wait()

    tp_start(TOKENS)
    for kind in (MIXER_IN, MIXER_OUT, SCALES):
        begin(kind)

    def small_step(hop, carry):
        for kind in (MIXER_IN, MIXER_OUT, SCALES):
            pump(kind, hop)
        return carry

    lax.fori_loop(1, far, small_step, 0)
    begin(GATE)
    begin(UP)
    small_step(far, 0)
    tp_start(OUT_ROWS)
    tp_wait(TOKENS)

    span = lower_ref.shape[1]
    groups = lower_ref.shape[0]

    def span_rows(i):
        return pl.ds(pl.multiple_of(i * span, span), span)

    def norm_span(i, gain_ref):
        here = span_rows(i)
        square = jnp.zeros((span, 1), jnp.float32)
        for t in range(n_tp):
            wide = tok_all[t, here, :].astype(jnp.float32)
            square += jnp.sum(wide * wide, axis=-1, keepdims=True)
        inverse = lax.rsqrt(square / (n_tp * own_width) + EPS)
        for f in range(n_fs):
            t, sub = f // per_own, f % per_own
            wide = tok_all[t, here, sub * block:(sub + 1) * block].astype(jnp.float32)
            gain = gain_ref[:, f * block:(f + 1) * block]
            normed[f, here, :] = (wide * inverse * gain).astype(jnp.bfloat16)

    def mixer_span(i, carry):
        here = span_rows(i)
        norm_span(i, pre_gain_ref)
        u_pre = v_pre = None
        for f in range(n_fs):
            source = normed[f, here, :]
            u_term = jnp.dot(source, uv_all[f, 0], preferred_element_type=jnp.float32)
            v_term = jnp.dot(source, uv_all[f, 1], preferred_element_type=jnp.float32)
            u_pre = u_term if f == 0 else u_pre + u_term
            v_pre = v_term if f == 0 else v_pre + v_term
        u_act = jax.nn.gelu(u_pre * u_scale_ref[...])
        v_act = jax.nn.gelu(v_pre * v_scale_ref[...])
        width = v_act.shape[1] // groups
        group_of = lax.broadcasted_iota(jnp.int32, v_act.shape, 1) // width
        centre = jnp.zeros_like(v_act)
        for g in range(groups):
            mean = jnp.sum(jnp.where(group_of == g, v_act, 0.0), axis=-1, keepdims=True) / width
            centre = jnp.where(group_of == g, mean, centre)
        apart = v_act - centre
        square = apart * apart
        inverse = jnp.zeros_like(v_act)
        for g in range(groups):
            spread = jnp.sum(jnp.where(group_of == g, square, 0.0), axis=-1, keepdims=True) / width
            inverse = jnp.where(group_of == g, lax.rsqrt(spread + EPS), inverse)
        v_norm = (apart * inverse * group_gain_ref[...]).astype(jnp.bfloat16)
        mixed = bias_ref[...]
        for g in range(groups):
            term = jnp.dot(lower_ref[g], v_norm, preferred_element_type=jnp.float32)
            mixed = mixed + jnp.where(group_of == g, term, 0.0)
        gated_all[tp, here, :] = (u_act * mixed).astype(jnp.bfloat16)
        return carry

    spans = rows // span
    lax.fori_loop(0, spans, mixer_span, 0)
    tp_start(GATED)
    pump(GATE, 1)
    tp_wait(OUT_ROWS)
    tp_wait(GATED)

    def resid_span(i, carry):
        here = span_rows(i)
        for f in range(n_fs):
            t, sub = f // per_own, f % per_own
            mix = None
            for s in range(n_tp):
                term = jnp.dot(gated_all[s, here, :], out_all[f, s],
                               preferred_element_type=jnp.float32)
                mix = term if s == 0 else mix + term
            mix = (mix * scale_all[f, 0:1, :]).astype(jnp.bfloat16)
            cols = slice(sub * block, (sub + 1) * block)
            tok_all[t, here, cols] = (
                tok_all[t, here, cols].astype(jnp.float32) + mix.astype(jnp.float32)
            ).astype(jnp.bfloat16)
        norm_span(i, ffn_gain_ref)
        return carry

    for k in range(1, n_tp):
        tp_copy(TOKENS, k, tp).wait_send()
    lax.fori_loop(0, spans, resid_span, 0)
    pump(UP, 1)

    chunk = span
    chunks = rows // chunk

    def fold(acc, weights, q):
        r, f = coords(q)

        def body(i, carry):
            here = pl.ds(pl.multiple_of(i * chunk, chunk), chunk)
            term = jnp.dot(normed[f, here, :], weights[q], preferred_element_type=jnp.float32)
            acc[r, here, :] = acc[r, here, :] + term
            return carry

        lax.fori_loop(0, chunks, body, 0)

    gate_acc[...] = jnp.zeros_like(gate_acc)
    up_acc[...] = jnp.zeros_like(up_acc)
    fold(gate_acc, gate_all, me)
    fold(up_acc, up_all, me)

    def fold_hop(acc, weights, kind, hop):
        for way in range(2):
            on(hop <= hops[kind][way],
               lambda way=way: fold(acc, weights, at_hop(way, hop)))

    def ffn_step(hop, carry):
        on(hop > 1, lambda: pump(GATE, hop))
        fold_hop(gate_acc, gate_all, GATE, hop)
        on(hop > 1, lambda: pump(UP, hop))

        def start_down():
            begin(DOWN_A)
            begin(DOWN_B)

        on(hop == far - 1, start_down)
        fold_hop(up_acc, up_all, UP, hop)
        return carry

    lax.fori_loop(1, far + 1, ffn_step, 0)

    def hidden_chunk(i, carry):
        here = pl.ds(pl.multiple_of(i * chunk, chunk), chunk)
        for r in range(n_rep):
            a = gate_acc[r, here, :] * gate_scale_ref[r:r + 1, :]
            b = up_acc[r, here, :] * up_scale_ref[r:r + 1, :]
            hidden[r, here, :] = (a / (1.0 + jnp.exp(-a)) * b).astype(jnp.bfloat16)
        return carry

    lax.fori_loop(0, chunks, hidden_chunk, 0)
    ffn_acc[...] = jnp.zeros_like(ffn_acc)

    def fold_down(q, low, size):
        r, f = coords(q)

        def body(i, carry):
            here = pl.ds(pl.multiple_of(i * chunk, chunk), chunk)
            term = jnp.dot(hidden[r, here, :], down_all[q], preferred_element_type=jnp.float32)
            ffn_acc[f, here, :] = ffn_acc[f, here, :] + term
            return carry

        lax.fori_loop(0, chunks, body, 0)

    def part_copy(f, owner, sender):
        sub = lax.rem(f, per_own)
        return pltpu.make_async_remote_copy(
            src_ref=part.at[f], dst_ref=parts_in.at[sender, sub], send_sem=part_send.at[f],
            recv_sem=part_recv.at[sender, sub], device_id={"tp": owner}, device_id_type=MESH)

    def finish(f):
        def body(i, carry):
            here = pl.ds(pl.multiple_of(i * chunk, chunk), chunk)
            part[f, here, :] = (ffn_acc[f, here, :] * scale_all[f, 1:2, :]).astype(jnp.bfloat16)
            return carry

        lax.fori_loop(0, chunks, body, 0)
        owner = f // per_own
        on(owner != tp, lambda: part_copy(f, owner, tp).start())

    def complete_at(f):
        last = 0
        for r in range(n_rep):
            gap = lax.rem(me - place(r, f) + n_ring, n_ring)
            last = jnp.maximum(last, jnp.minimum(gap, n_ring - gap))
        return last

    fold_down(me, 0, down_rows)

    def down_step(hop, carry):
        pump(DOWN_A, hop)
        pump(DOWN_B, hop)
        fold_down(at_hop(0, hop), 0, down_rows)
        on(hop <= near, lambda: fold_down(at_hop(1, hop), 0, down_rows))

        def finish_if(f, inner):
            on(complete_at(f) == hop, lambda: finish(f))
            return inner

        lax.fori_loop(0, n_fs, finish_if, 0)
        return carry

    lax.fori_loop(1, far + 1, down_step, 0)

    for k in range(1, n_tp):
        sender = lax.rem(tp + k, n_tp)
        for sub in range(per_own):
            part_copy(tp * per_own + sub, tp, sender).wait_recv()

    def close_span(i, carry):
        here = pl.ds(pl.multiple_of(i * chunk, chunk), chunk)
        for sub in range(per_own):
            cols = slice(sub * block, (sub + 1) * block)
            total = part[tp * per_own + sub, here, :].astype(jnp.float32)
            for k in range(1, n_tp):
                total += parts_in[lax.rem(tp + k, n_tp), sub, here, :].astype(jnp.float32)
            total = total.astype(jnp.bfloat16).astype(jnp.float32)
            kept = tok_all[tp, here, cols].astype(jnp.float32)
            result_ref[here, cols] = (kept + total).astype(jnp.bfloat16)
        return carry

    lax.fori_loop(0, chunks, close_span, 0)

    for kind in range(KINDS):
        for way in range(2):
            def sent(hop, carry, kind=kind, way=way):
                send(kind, way, hop).wait_send()
                return carry

            lax.fori_loop(1, hops[kind][way] + 1, sent, 0)
    for kind in (OUT_ROWS, GATED):
        for k in range(1, n_tp):
            tp_copy(kind, k, tp).wait_send()

    def part_sent(f, carry):
        owner = f // per_own
        on(owner != tp, lambda: part_copy(f, owner, tp).wait_send())
        return carry

    lax.fori_loop(0, n_fs, part_sent, 0)


def shards(
    sizes,
    tokens,
    pre_gain,
    u_weight,
    u_scale,
    v_weight,
    v_scale,
    group_gain,
    span_weight,
    span_bias,
    out_weight,
    out_scale,
    ffn_gain,
    gate_weight,
    gate_scale,
    up_weight,
    up_scale,
    down_weight,
    down_scale,
):
    n_rep, n_fs, n_tp = sizes
    n_ring = n_rep * n_fs
    rep = lax.axis_index("rep")

    def share(array, axis):
        width = array.shape[axis] // n_rep
        return lax.dynamic_slice_in_dim(array, rep * width, width, axis).astype(jnp.bfloat16)

    rows, own_width = tokens.shape
    block, local_hidden = gate_weight.shape
    hid = local_hidden // n_rep
    channels = u_weight.shape[1]
    groups, span = span_weight.shape[0], span_weight.shape[1]
    uv = share(jnp.stack([u_weight, v_weight]), 1)
    scales = jnp.stack([out_scale, down_scale])
    bias = jnp.repeat(jnp.transpose(span_bias), channels // groups, axis=1)
    row = lambda vector: vector.reshape(1, -1)
    operands = (
        tokens, scales, uv, share(out_weight, 0), share(gate_weight, 1), share(up_weight, 1),
        share(down_weight, 0), row(pre_gain), row(ffn_gain), row(u_scale), row(v_scale),
        row(group_gain), jnp.tril(span_weight), bias, gate_scale.reshape(n_rep, hid),
        up_scale.reshape(n_rep, hid),
    )
    hbm, vmem = pl.BlockSpec(memory_space=pl.ANY), pl.BlockSpec(memory_space=pltpu.VMEM)
    bf16, f32 = jnp.bfloat16, jnp.float32
    per_own = own_width // block
    steps = n_ring // 2
    return pl.pallas_call(
        functools.partial(layer_kernel, sizes),
        out_shape=jax.ShapeDtypeStruct((rows, own_width), bf16),
        in_specs=[hbm] * 7 + [vmem] * 9,
        out_specs=vmem,
        scratch_shapes=[
            pltpu.VMEM((n_tp, rows, own_width), bf16),
            pltpu.VMEM((n_ring, 2, block), f32),
            pltpu.VMEM((n_fs, 2, block, channels), bf16),
            pltpu.VMEM((n_fs, n_tp, channels, block), bf16),
            pltpu.VMEM((n_ring, block, hid), bf16),
            pltpu.VMEM((n_ring, block, hid), bf16),
            pltpu.VMEM((n_ring, hid, block), bf16),
            pltpu.VMEM((n_fs, rows, block), bf16),
            pltpu.VMEM((n_tp, rows, channels), bf16),
            pltpu.VMEM((n_rep, rows, hid), f32),
            pltpu.VMEM((n_rep, rows, hid), f32),
            pltpu.VMEM((n_rep, rows, hid), bf16),
            pltpu.VMEM((n_fs, rows, block), f32),
            pltpu.VMEM((n_fs, rows, block), bf16),
            pltpu.VMEM((n_tp, per_own, rows, block), bf16),
            pltpu.SemaphoreType.DMA((7,)),
            pltpu.SemaphoreType.DMA((KINDS, 2, steps)),
            pltpu.SemaphoreType.DMA((KINDS, 2, steps)),
            pltpu.SemaphoreType.DMA((3, n_tp - 1)),
            pltpu.SemaphoreType.DMA((3, n_tp - 1)),
            pltpu.SemaphoreType.DMA((n_fs,)),
            pltpu.SemaphoreType.DMA((n_tp, per_own)),
        ],
        compiler_params=pltpu.CompilerParams(
            collective_id=0, has_side_effects=True, vmem_limit_bytes=62 * 1024 * 1024
        ),
    )(*operands)


def solution(mesh):
    placed = (
        P(("rep", "fs"), "tp"),
        P(),
        P("fs", "tp"),
        P("tp"),
        P("fs", "tp"),
        P("tp"),
        P("tp"),
        P("tp", None, None),
        P("tp", None),
        P("tp", "fs"),
        P("fs"),
        P(),
        P("fs", "tp"),
        P("tp"),
        P("fs", "tp"),
        P("tp"),
        P("tp", "fs"),
        P("fs"),
    )
    sizes = (mesh.shape["rep"], mesh.shape["fs"], mesh.shape["tp"])
    return jax.shard_map(
        functools.partial(shards, sizes), mesh=mesh, in_specs=placed, out_specs=P(("rep", "fs"), "tp"), check_vma=False
    )
```

```python
import functools

import jax
import jax.numpy as jnp
from jax import lax
from jax.experimental import pallas as pl
from jax.experimental.pallas import tpu as pltpu
from jax.sharding import PartitionSpec as P

EPS = 0.02
MESH = pl.DeviceIdType.MESH
SCALES, MIXER_IN, MIXER_OUT, GATE, UP, DOWN_A, DOWN_B = range(7)
KINDS = 7
TOKENS, OUT_ROWS, GATED = range(3)


def layer_kernel(
    sizes,
    tokens_ref,
    out_scale_ref,
    down_scale_ref,
    uv_ref,
    out_ref,
    gate_ref,
    up_ref,
    down_ref,
    pre_gain_ref,
    ffn_gain_ref,
    u_scale_ref,
    v_scale_ref,
    group_gain_ref,
    lower_ref,
    bias_ref,
    gate_scale_ref,
    up_scale_ref,
    result_ref,
    tok_all,
    scale_all,
    uv_all,
    out_all,
    gate_all,
    up_all,
    down_all,
    normed,
    gated_all,
    gate_acc,
    up_acc,
    hidden,
    ffn_acc,
    part,
    parts_in,
    local_sem,
    line_send,
    line_recv,
    rep_send,
    rep_recv,
    tp_send,
    tp_recv,
    part_send,
    part_recv,
):
    n_rep, n_fs, n_tp = sizes
    rows, own_width = tokens_ref.shape
    block = normed.shape[2]
    per_own = own_width // block
    rep, fs, tp = lax.axis_index("rep"), lax.axis_index("fs"), lax.axis_index("tp")

    last_hop = n_fs - 1

    def at_hop(way, hop):
        return fs - hop if way == 0 else fs + hop

    def arrives(way, hop):
        f = at_hop(way, hop)
        return jnp.logical_and(f >= 0, f < n_fs)

    def leaves(way, hop):
        ahead = fs + 1 if way == 0 else fs - 1
        return jnp.logical_and(arrives(way, hop - 1), jnp.logical_and(ahead >= 0, ahead < n_fs))

    uv_rows, out_rows, down_rows = uv_ref.shape[2], out_ref.shape[1], down_ref.shape[1]
    half = down_rows // 2

    def slot(kind, r, f):
        if kind == SCALES:
            return scale_all.at[f]
        if kind == MIXER_IN:
            return uv_all.at[f, :, pl.ds(pl.multiple_of(r * uv_rows, uv_rows), uv_rows)]
        if kind == MIXER_OUT:
            return out_all.at[f, tp, pl.ds(pl.multiple_of(r * out_rows, out_rows), out_rows)]
        if kind == GATE:
            return gate_all.at[r, f]
        if kind == UP:
            return up_all.at[r, f]
        return down_all.at[r, f, pl.ds(0 if kind == DOWN_A else half, half)]

    def line_copy(kind, way, hop, f):
        ref = slot(kind, rep, f)
        return pltpu.make_async_remote_copy(
            src_ref=ref, dst_ref=ref, send_sem=line_send.at[kind, way, hop - 1],
            recv_sem=line_recv.at[kind, way, hop - 1],
            device_id={"fs": fs + 1 if way == 0 else fs - 1}, device_id_type=MESH)

    def send(kind, way, hop):
        return line_copy(kind, way, hop, at_hop(way, hop - 1))

    def rep_copy(kind, way, hop, k, r):
        ref = slot(kind, r, at_hop(way, hop))
        return pltpu.make_async_remote_copy(
            src_ref=ref, dst_ref=ref, send_sem=rep_send.at[kind, way, hop - 1, k - 1],
            recv_sem=rep_recv.at[kind, way, hop - 1, k - 1],
            device_id={"rep": lax.rem(rep + k, n_rep)}, device_id_type=MESH)

    def on(condition, action):
        if isinstance(condition, bool):
            if condition:
                action()
        else:
            pl.when(condition)(action)

    def begin(kind):
        for way in range(2):
            on(leaves(way, 1), lambda way=way: send(kind, way, 1).start())

    def pump(kind, hop):
        for way in range(2):
            def take(way=way):
                line_copy(kind, way, hop, at_hop(way, hop)).wait_recv()
                on(leaves(way, hop + 1), lambda: send(kind, way, hop + 1).start())
                if kind != SCALES:
                    for k in range(1, n_rep):
                        rep_copy(kind, way, hop, k, rep).start()
            on(arrives(way, hop), take)

    def rep_wait(kind, hop):
        for way in range(2):
            def take(way=way):
                for k in range(1, n_rep):
                    rep_copy(kind, way, hop, k, lax.rem(rep - k + n_rep, n_rep)).wait_recv()
            on(arrives(way, hop), take)

    def tp_ref(kind, t):
        if kind == TOKENS:
            return tok_all.at[t]
        if kind == OUT_ROWS:
            return out_all.at[:, t]
        return gated_all.at[t]

    def tp_copy(kind, k, t):
        ref = tp_ref(kind, t)
        return pltpu.make_async_remote_copy(
            src_ref=ref, dst_ref=ref, send_sem=tp_send.at[kind, k - 1],
            recv_sem=tp_recv.at[kind, k - 1], device_id={"tp": lax.rem(tp + k, n_tp)},
            device_id_type=MESH)

    def tp_start(kind):
        for k in range(1, n_tp):
            tp_copy(kind, k, tp).start()

    def tp_wait(kind):
        for k in range(1, n_tp):
            tp_copy(kind, k, lax.rem(tp - k + n_tp, n_tp)).wait_recv()

    own = [
        pltpu.make_async_copy(tokens_ref, tok_all.at[tp], local_sem.at[0]),
        pltpu.make_async_copy(out_scale_ref, scale_all.at[fs, 0], local_sem.at[1]),
        pltpu.make_async_copy(down_scale_ref, scale_all.at[fs, 1], local_sem.at[2]),
    ]
    pairs = [(MIXER_IN, lambda r: uv_ref.at[r]), (MIXER_OUT, lambda r: out_ref.at[r]),
             (GATE, lambda r: gate_ref.at[r]), (UP, lambda r: up_ref.at[r]),
             (DOWN_A, lambda r: down_ref.at[r, pl.ds(0, half)]),
             (DOWN_B, lambda r: down_ref.at[r, pl.ds(half, half)])]
    for i, (kind, source) in enumerate(pairs):
        for r in range(n_rep):
            own.append(pltpu.make_async_copy(
                source(r), slot(kind, r, fs), local_sem.at[3 + i * n_rep + r]))
    for copy in own:
        copy.start()
    barrier = pltpu.get_barrier_semaphore()
    for way in range(2):
        def greet(way=way):
            pl.semaphore_signal(barrier, inc=1, device_id={"fs": fs + 1 if way == 0 else fs - 1},
                                device_id_type=MESH)
        on(leaves(way, 1), greet)
    for k in range(1, n_rep):
        pl.semaphore_signal(barrier, inc=1, device_id={"rep": lax.rem(rep + k, n_rep)},
                            device_id_type=MESH)
    for k in range(1, n_tp):
        pl.semaphore_signal(barrier, inc=1, device_id={"tp": lax.rem(tp + k, n_tp)},
                            device_id_type=MESH)
    beside = (fs > 0).astype(jnp.int32) + (fs < n_fs - 1).astype(jnp.int32)
    pl.semaphore_wait(barrier, beside + n_rep - 1 + n_tp - 1)
    for copy in own:
        copy.wait()

    tp_start(TOKENS)
    small = (MIXER_IN, MIXER_OUT, SCALES)
    for kind in small:
        begin(kind)
    begin(GATE)

    def small_step(hop, carry):
        for kind in small:
            pump(kind, hop)
        return carry

    small_step(1, 0)
    begin(UP)
    small_step(2, 0)
    pump(GATE, 1)
    lax.fori_loop(3, last_hop + 1, small_step, 0)

    def small_rep(hop, carry):
        for kind in (MIXER_IN, MIXER_OUT):
            rep_wait(kind, hop)
        return carry

    lax.fori_loop(1, last_hop + 1, small_rep, 0)
    tp_start(OUT_ROWS)
    tp_wait(TOKENS)

    span = lower_ref.shape[1]
    groups = lower_ref.shape[0]

    def span_rows(i):
        return pl.ds(pl.multiple_of(i * span, span), span)

    def norm_span(i, gain_ref):
        here = span_rows(i)
        square = jnp.zeros((span, 1), jnp.float32)
        for t in range(n_tp):
            wide = tok_all[t, here, :].astype(jnp.float32)
            square += jnp.sum(wide * wide, axis=-1, keepdims=True)
        inverse = lax.rsqrt(square / (n_tp * own_width) + EPS)
        for f in range(n_fs):
            t, sub = f // per_own, f % per_own
            wide = tok_all[t, here, sub * block:(sub + 1) * block].astype(jnp.float32)
            gain = gain_ref[:, f * block:(f + 1) * block]
            normed[f, here, :] = (wide * inverse * gain).astype(jnp.bfloat16)

    def lower_part(g):
        square = lower_ref[g].astype(jnp.float32)
        t = lax.broadcasted_iota(jnp.int32, square.shape, 0)
        s = lax.broadcasted_iota(jnp.int32, square.shape, 1)
        return jnp.where(s <= t, square, 0.0).astype(jnp.bfloat16)

    def mixer_span(i, carry):
        here = span_rows(i)
        norm_span(i, pre_gain_ref)
        u_pre = v_pre = None
        for f in range(n_fs):
            source = normed[f, here, :]
            u_term = jnp.dot(source, uv_all[f, 0], preferred_element_type=jnp.float32)
            v_term = jnp.dot(source, uv_all[f, 1], preferred_element_type=jnp.float32)
            u_pre = u_term if f == 0 else u_pre + u_term
            v_pre = v_term if f == 0 else v_pre + v_term
        u_act = jax.nn.gelu(u_pre * u_scale_ref[...])
        v_act = jax.nn.gelu(v_pre * v_scale_ref[...])
        width = v_act.shape[1] // groups
        group_of = lax.broadcasted_iota(jnp.int32, v_act.shape, 1) // width
        centre = jnp.zeros_like(v_act)
        for g in range(groups):
            mean = jnp.sum(jnp.where(group_of == g, v_act, 0.0), axis=-1, keepdims=True) / width
            centre = jnp.where(group_of == g, mean, centre)
        apart = v_act - centre
        square = apart * apart
        inverse = jnp.zeros_like(v_act)
        for g in range(groups):
            spread = jnp.sum(jnp.where(group_of == g, square, 0.0), axis=-1, keepdims=True) / width
            inverse = jnp.where(group_of == g, lax.rsqrt(spread + EPS), inverse)
        v_norm = (apart * inverse * group_gain_ref[...]).astype(jnp.bfloat16)
        mixed = bias_ref[...]
        for g in range(groups):
            term = jnp.dot(lower_part(g), v_norm, preferred_element_type=jnp.float32)
            mixed = mixed + jnp.where(group_of == g, term, 0.0)
        gated_all[tp, here, :] = (u_act * mixed).astype(jnp.bfloat16)
        return carry

    spans = rows // span
    lax.fori_loop(0, spans, mixer_span, 0)
    tp_start(GATED)
    pump(UP, 1)
    tp_wait(OUT_ROWS)
    tp_wait(GATED)

    def resid_span(i, carry):
        here = span_rows(i)
        for f in range(n_fs):
            t, sub = f // per_own, f % per_own
            mix = None
            for s in range(n_tp):
                term = jnp.dot(gated_all[s, here, :], out_all[f, s],
                               preferred_element_type=jnp.float32)
                mix = term if s == 0 else mix + term
            mix = (mix * scale_all[f, 0]).astype(jnp.bfloat16)
            cols = slice(sub * block, (sub + 1) * block)
            tok_all[t, here, cols] = (
                tok_all[t, here, cols].astype(jnp.float32) + mix.astype(jnp.float32)
            ).astype(jnp.bfloat16)
        norm_span(i, ffn_gain_ref)
        return carry

    for k in range(1, n_tp):
        tp_copy(TOKENS, k, tp).wait_send()
    lax.fori_loop(0, spans, resid_span, 0)

    chunk = span
    chunks = rows // chunk

    def fold(acc, weights, r, f):
        def body(i, carry):
            here = pl.ds(pl.multiple_of(i * chunk, chunk), chunk)
            term = jnp.dot(normed[f, here, :], weights[r, f], preferred_element_type=jnp.float32)
            acc[r, here, :] = acc[r, here, :] + term
            return carry

        lax.fori_loop(0, chunks, body, 0)

    def others():
        return [lax.rem(rep + k, n_rep) for k in range(1, n_rep)]

    def fold_hop(acc, weights, reps, hop):
        for way in range(2):
            def both(way=way):
                for r in reps:
                    fold(acc, weights, r, at_hop(way, hop))
            on(arrives(way, hop), both)

    gate_acc[...] = jnp.zeros_like(gate_acc)
    up_acc[...] = jnp.zeros_like(up_acc)
    for r in range(n_rep):
        fold(gate_acc, gate_all, r, fs)
        fold(up_acc, up_all, r, fs)

    def ffn_step(hop, carry):
        on(hop > 1, lambda: pump(GATE, hop))
        fold_hop(gate_acc, gate_all, [rep], hop)

        def late_up():
            rep_wait(UP, hop - 1)
            fold_hop(up_acc, up_all, others(), hop - 1)

        on(hop > 1, late_up)
        on(hop > 1, lambda: pump(UP, hop))

        def start_down():
            begin(DOWN_A)
            begin(DOWN_B)

        on(hop == last_hop - 1, start_down)
        fold_hop(up_acc, up_all, [rep], hop)
        rep_wait(GATE, hop)
        fold_hop(gate_acc, gate_all, others(), hop)
        return carry

    lax.fori_loop(1, last_hop + 1, ffn_step, 0)
    rep_wait(UP, last_hop)
    fold_hop(up_acc, up_all, others(), last_hop)

    hid = hidden.shape[2]

    def hidden_chunk(i, carry):
        here = pl.ds(pl.multiple_of(i * chunk, chunk), chunk)
        for r in range(n_rep):
            a = gate_acc[r, here, :] * gate_scale_ref[:, r * hid:(r + 1) * hid]
            b = up_acc[r, here, :] * up_scale_ref[:, r * hid:(r + 1) * hid]
            hidden[r, here, :] = (a / (1.0 + jnp.exp(-a)) * b).astype(jnp.bfloat16)
        return carry

    lax.fori_loop(0, chunks, hidden_chunk, 0)
    ffn_acc[...] = jnp.zeros_like(ffn_acc)

    def fold_down(r, f):
        def body(i, carry):
            here = pl.ds(pl.multiple_of(i * chunk, chunk), chunk)
            term = jnp.dot(hidden[r, here, :], down_all[r, f], preferred_element_type=jnp.float32)
            ffn_acc[f, here, :] = ffn_acc[f, here, :] + term
            return carry

        lax.fori_loop(0, chunks, body, 0)

    def part_copy(f, owner, sender):
        sub = lax.rem(f, per_own)
        return pltpu.make_async_remote_copy(
            src_ref=part.at[f], dst_ref=parts_in.at[sender, sub], send_sem=part_send.at[f],
            recv_sem=part_recv.at[sender, sub], device_id={"tp": owner}, device_id_type=MESH)

    def finish(f):
        def body(i, carry):
            here = pl.ds(pl.multiple_of(i * chunk, chunk), chunk)
            part[f, here, :] = (ffn_acc[f, here, :] * scale_all[f, 1]).astype(jnp.bfloat16)
            return carry

        lax.fori_loop(0, chunks, body, 0)
        owner = f // per_own
        on(owner != tp, lambda: part_copy(f, owner, tp).start())

    def down_own(hop):
        for way in range(2):
            on(arrives(way, hop), lambda way=way: fold_down(rep, at_hop(way, hop)))

    def down_others(hop):
        rep_wait(DOWN_B, hop)
        for way in range(2):
            def close(way=way):
                for r in others():
                    fold_down(r, at_hop(way, hop))
                finish(at_hop(way, hop))
            on(arrives(way, hop), close)

    pump(DOWN_A, 1)
    for r in range(n_rep):
        fold_down(r, fs)
    finish(fs)

    def down_step(hop, carry):
        on(hop > 1, lambda: pump(DOWN_A, hop))
        on(hop > 1, lambda: down_others(hop - 1))
        pump(DOWN_B, hop)
        down_own(hop)
        rep_wait(DOWN_A, hop)
        return carry

    lax.fori_loop(1, last_hop + 1, down_step, 0)
    down_others(last_hop)

    for k in range(1, n_tp):
        sender = lax.rem(tp + k, n_tp)
        for sub in range(per_own):
            part_copy(tp * per_own + sub, tp, sender).wait_recv()

    def close_span(i, carry):
        here = pl.ds(pl.multiple_of(i * chunk, chunk), chunk)
        for sub in range(per_own):
            cols = slice(sub * block, (sub + 1) * block)
            total = part[tp * per_own + sub, here, :].astype(jnp.float32)
            for k in range(1, n_tp):
                total += parts_in[lax.rem(tp + k, n_tp), sub, here, :].astype(jnp.float32)
            total = total.astype(jnp.bfloat16).astype(jnp.float32)
            kept = tok_all[tp, here, cols].astype(jnp.float32)
            result_ref[here, cols] = (kept + total).astype(jnp.bfloat16)
        return carry

    lax.fori_loop(0, chunks, close_span, 0)

    for kind in range(KINDS):
        for way in range(2):
            def sent(hop, carry, kind=kind, way=way):
                on(leaves(way, hop), lambda: send(kind, way, hop).wait_send())
                if kind != SCALES:
                    def rep_sent():
                        for k in range(1, n_rep):
                            rep_copy(kind, way, hop, k, rep).wait_send()
                    on(arrives(way, hop), rep_sent)
                return carry

            lax.fori_loop(1, last_hop + 1, sent, 0)
    for kind in (OUT_ROWS, GATED):
        for k in range(1, n_tp):
            tp_copy(kind, k, tp).wait_send()

    def part_sent(f, carry):
        owner = f // per_own
        on(owner != tp, lambda: part_copy(f, owner, tp).wait_send())
        return carry

    lax.fori_loop(0, n_fs, part_sent, 0)


def shards(
    sizes,
    tokens,
    pre_gain,
    u_weight,
    u_scale,
    v_weight,
    v_scale,
    group_gain,
    span_weight,
    span_bias,
    out_weight,
    out_scale,
    ffn_gain,
    gate_weight,
    gate_scale,
    up_weight,
    up_scale,
    down_weight,
    down_scale,
):
    n_rep, n_fs, n_tp = sizes
    bf16, f32 = jnp.bfloat16, jnp.float32

    def halves(array, axis):
        shape = array.shape
        split = shape[:axis] + (n_rep, shape[axis] // n_rep) + shape[axis + 1:]
        return jnp.moveaxis(array.astype(bf16).reshape(split), axis, 0)

    rows, own_width = tokens.shape
    block, local_hidden = gate_weight.shape
    hid = local_hidden // n_rep
    channels = u_weight.shape[1]
    groups, span = span_weight.shape[0], span_weight.shape[1]
    uv = halves(jnp.stack([u_weight, v_weight]), 1)
    bias = jnp.repeat(jnp.transpose(span_bias), channels // groups, axis=1)
    row = lambda vector: vector.reshape(1, -1)
    operands = (
        tokens, row(out_scale), row(down_scale), uv, halves(out_weight, 0), halves(gate_weight, 1), halves(up_weight, 1),
        halves(down_weight, 0), row(pre_gain), row(ffn_gain), row(u_scale), row(v_scale),
        row(group_gain), span_weight, bias, row(gate_scale),
        row(up_scale),
    )
    hbm, vmem = pl.BlockSpec(memory_space=pl.ANY), pl.BlockSpec(memory_space=pltpu.VMEM)
    per_own = own_width // block
    steps = n_fs - 1
    return pl.pallas_call(
        functools.partial(layer_kernel, sizes),
        out_shape=jax.ShapeDtypeStruct((rows, own_width), bf16),
        in_specs=[hbm] * 8 + [vmem] * 9,
        out_specs=vmem,
        scratch_shapes=[
            pltpu.VMEM((n_tp, rows, own_width), bf16),
            pltpu.VMEM((n_fs, 2, 1, block), f32),
            pltpu.VMEM((n_fs, 2, block, channels), bf16),
            pltpu.VMEM((n_fs, n_tp, channels, block), bf16),
            pltpu.VMEM((n_rep, n_fs, block, hid), bf16),
            pltpu.VMEM((n_rep, n_fs, block, hid), bf16),
            pltpu.VMEM((n_rep, n_fs, hid, block), bf16),
            pltpu.VMEM((n_fs, rows, block), bf16),
            pltpu.VMEM((n_tp, rows, channels), bf16),
            pltpu.VMEM((n_rep, rows, hid), f32),
            pltpu.VMEM((n_rep, rows, hid), f32),
            pltpu.VMEM((n_rep, rows, hid), bf16),
            pltpu.VMEM((n_fs, rows, block), f32),
            pltpu.VMEM((n_fs, rows, block), bf16),
            pltpu.VMEM((n_tp, per_own, rows, block), bf16),
            pltpu.SemaphoreType.DMA((3 + 6 * n_rep,)),
            pltpu.SemaphoreType.DMA((KINDS, 2, steps)),
            pltpu.SemaphoreType.DMA((KINDS, 2, steps)),
            pltpu.SemaphoreType.DMA((KINDS, 2, steps, n_rep - 1)),
            pltpu.SemaphoreType.DMA((KINDS, 2, steps, n_rep - 1)),
            pltpu.SemaphoreType.DMA((3, n_tp - 1)),
            pltpu.SemaphoreType.DMA((3, n_tp - 1)),
            pltpu.SemaphoreType.DMA((n_fs,)),
            pltpu.SemaphoreType.DMA((n_tp, per_own)),
        ],
        compiler_params=pltpu.CompilerParams(
            collective_id=0, has_side_effects=True, vmem_limit_bytes=62 * 1024 * 1024
        ),
    )(*operands)


def solution(mesh):
    placed = (
        P(("rep", "fs"), "tp"),
        P(),
        P("fs", "tp"),
        P("tp"),
        P("fs", "tp"),
        P("tp"),
        P("tp"),
        P("tp", None, None),
        P("tp", None),
        P("tp", "fs"),
        P("fs"),
        P(),
        P("fs", "tp"),
        P("tp"),
        P("fs", "tp"),
        P("tp"),
        P("tp", "fs"),
        P("fs"),
    )
    sizes = (mesh.shape["rep"], mesh.shape["fs"], mesh.shape["tp"])
    return jax.shard_map(
        functools.partial(shards, sizes), mesh=mesh, in_specs=placed, out_specs=P(("rep", "fs"), "tp"), check_vma=False
    )
```
